32 devices in a mesh: ep: 16 (over z, y, x), tp: 2 (over core).
Axes of the slice: x: 2, y: 2, z: 4, core: 2. Of those that a mesh axis runs over, the one named last changes fastest.
Arguments:
- tokens: bfloat16 [256, 2048], P('ep', 'tp'), may hold values from -6 to 6
- state: float32 [256, 4, 128, 128], P('ep', 'tp'), may hold values from -4 to 4
- norm_mix: float32 [2048], replicated, may hold values from 0.1 to 1.9
- w_query: bfloat16 [2048, 512], P(None, 'tp'), may hold values from -0.125 to 0.125
- w_key: bfloat16 [2048, 512], P(None, 'tp'), may hold values from -0.125 to 0.125
- w_value: bfloat16 [2048, 512], P(None, 'tp'), may hold values from -0.125 to 0.125
- w_out: bfloat16 [512, 2048], P('tp'), may hold values from -0.25 to 0.25
- norm_ffn: float32 [2048], P('tp'), may hold values from 0.1 to 1.9
- gate_vector: bfloat16 [2048], P('tp'), may hold values from -0.125 to 0.125
- dense_gate: bfloat16 [2048, 2816], P('tp', 'ep'), may hold values from -0.125 to 0.125
- dense_up: bfloat16 [2048, 2816], P('tp', 'ep'), may hold values from -0.125 to 0.125
- dense_down: bfloat16 [2816, 2048], P('ep', 'tp'), may hold values from -0.109375 to 0.109375
- exp_gate: bfloat16 [16, 2048, 1408], P('ep', None, 'tp'), may hold values from -0.125 to 0.125
- exp_up: bfloat16 [16, 2048, 1408], P('ep', None, 'tp'), may hold values from -0.125 to 0.125
- exp_down: bfloat16 [16, 1408, 2048], P('ep', 'tp'), may hold values from -0.109375 to 0.109375
- routes: int32 [256, 2], P('ep'), may hold values from 0 to 7, all different within a row; in each aligned block of 16 rows (0 to 15, 16 to 31, ...) at most 5 rows name the same one
- route_w: bfloat16 [256, 2], P('ep'), may hold values from 0.099609375 to 1
Outputs:
- mixed: bfloat16 [256, 2048], P('ep', 'tp')
- new_state: float32 [256, 4, 128, 128], P('ep', 'tp')
The draws below stay inside these ranges and needn't reach their ends.
Inputs may be any that keep to these rules, and one draw needn't show every extreme that they name: `routes`: each row names 2 different experts. Within the rows of one device (aligned blocks of 16 rows) no expert is named by more than 5 rows, a bound that some blocks reach.
All inputs are finite; a program needn't handle non-finite values.
Results may differ from the reference program's by a relative error of at most 0.014.
Values may be sent and summed in bfloat16 or wider, within the bound.
A program may use at most 128 MiB of HBM per device.

```python
import math
import jax
import jax.numpy as jnp
import numpy as np
from jax import lax

D = 2048
HEADS = 4
HEAD = 128
FF = 2816
FF_D = 2816
EXPERTS = 8
TOPK = 2
SEQ_DEV = 16
CAP = 5
E_SPLIT = 2
TOKENS = 256
N_EP = 16
N_TP = 2


def levels(own_key, shape, pieces, low, largest):
    level = 1.0
    for dim, blocks in pieces:
        draws = jax.random.uniform(jax.random.fold_in(jax.random.fold_in(own_key, 6), dim), (blocks,), jnp.float32, low / len(pieces), largest / len(pieces))
        level = level * jnp.repeat(jnp.exp(draws), shape[dim] // blocks).reshape((-1,) + (1,) * (len(shape) - 1 - dim))
    return level


def shared_out(own_key, own, number, rows, count, top, reach, lean):
    order = jax.random.permutation(own_key, count)
    packed, usual = shares(count, rows * top, reach, lean, True), shares(count, rows * top, reach, lean, False)
    places = jnp.arange(count)

    def named(lengths, turn):
        used = int((lengths > 0).sum())
        fixed = max(1, used // 4)
        moved = fixed + (places - fixed + turn * (used - fixed)) % max(1, count - fixed)
        return jnp.zeros((count,), jnp.int32).at[order[jnp.where(places < fixed, places, moved)]].set(jnp.asarray(lengths, jnp.int32))

    lengths = jnp.where(number % 4 == 0, named(packed, number // 4), named(usual, number - number // 4 - 1))
    mixed = jax.random.permutation(jax.random.fold_in(own, 3), count)
    donor, taker = mixed[0:count // 2 * 2:2], mixed[1:count // 2 * 2:2]
    slack = jnp.minimum(lengths[donor] - 1, reach - lengths[taker]) // 2
    slack = jnp.where((donor == order[0]) | (taker == order[0]) | (lengths[taker] == 0), 0, jnp.maximum(slack, 0))
    moved = jax.random.randint(jax.random.fold_in(own, 4), (count // 2,), 0, 1 << 20) % (slack + 1)
    lengths = lengths.at[donor].add(-moved).at[taker].add(moved)
    labels = jnp.searchsorted(jnp.cumsum(lengths), jnp.arange(rows * top), side="right").astype(jnp.int32)
    listing = labels.reshape(top, rows).T
    listing = listing[jax.random.permutation(jax.random.fold_in(own, 1), rows)]
    turn = jax.random.randint(jax.random.fold_in(own, 2), (rows, 1), 0, top)
    return jnp.take_along_axis(listing, (jnp.arange(top)[None, :] + turn) % top, axis=1)


def shares(number_of, total, bound, slope, full):
    loads = [(1 << 20) // math.isqrt(grade ** slope) + 1 for grade in range(1, number_of + 1)]
    largest = bound if full else min(bound, max(-(-total // number_of), total * loads[0] // sum(loads)))
    least = 1 if total - largest >= number_of - 1 else 0
    counts, spare = [largest] + [least] * (number_of - 1), total - largest - least * (number_of - 1)
    while spare > 0:
        free = [i for i in range(1, number_of) if counts[i] < largest] or [i for i in range(1, number_of) if counts[i] < bound]
        whole, left = sum([loads[i] for i in free]), spare
        for i in free:
            extra = min(bound - counts[i], max(1, left * loads[i] // whole), spare)
            counts[i] = counts[i] + extra
            spare = spare - extra
    return np.array(counts)


def gaussian(own_key, dims, scale, bound, cuts=(), kind=jnp.bfloat16):
    level = levels(own_key, dims, cuts, -0.22, 0.18) if cuts else 1.0
    entries = jax.random.normal(own_key, dims, jnp.float32) * scale * level
    return jnp.minimum(jnp.maximum(entries, -bound), bound).astype(kind)


def setup_inputs(seed: int = 0) -> dict:
    seeds = jax.random.split(jax.random.key(seed), 18)
    tokens = gaussian(seeds[0], (TOKENS, D), 1.0, 6.0, ((0, 16), (1, 2)))
    state = gaussian(seeds[1], (TOKENS, HEADS, HEAD, HEAD), 0.5, 4.0, ((0, 16), (1, 2)), jnp.float32)
    norm_mix = jnp.clip(1.0 + 0.18 * jax.random.normal(seeds[2], (D,), jnp.float32), 0.1, 1.9)
    w_query = gaussian(seeds[3], (D, HEADS * HEAD), D ** -0.5, 0.125, ((1, 2),))
    w_key = gaussian(seeds[4], (D, HEADS * HEAD), D ** -0.5, 0.125, ((1, 2),))
    w_value = gaussian(seeds[5], (D, HEADS * HEAD), D ** -0.5, 0.125, ((1, 2),))
    w_out = gaussian(seeds[6], (HEADS * HEAD, D), (HEADS * HEAD) ** -0.5, 0.25, ((0, 2),))
    norm_ffn = jnp.clip(1.0 + 0.18 * jax.random.normal(seeds[7], (D,), jnp.float32), 0.1, 1.9)
    gate_vector = gaussian(seeds[8], (D,), D ** -0.5, 0.125, ((0, 2),))
    dense_gate = gaussian(seeds[9], (D, FF_D), D ** -0.5, 0.125, ((0, 2), (1, 16)))
    dense_up = gaussian(seeds[10], (D, FF_D), D ** -0.5, 0.125, ((0, 2), (1, 16)))
    dense_down = gaussian(seeds[11], (FF_D, D), FF_D ** -0.5, 0.109375, ((0, 16), (1, 2)))
    exp_gate = gaussian(seeds[12], (EXPERTS * E_SPLIT, D, FF // E_SPLIT), D ** -0.5, 0.125, ((0, 16), (2, 2)))
    exp_up = gaussian(seeds[13], (EXPERTS * E_SPLIT, D, FF // E_SPLIT), D ** -0.5, 0.125, ((0, 16), (2, 2)))
    exp_down = gaussian(seeds[14], (EXPERTS * E_SPLIT, FF // E_SPLIT, D), FF ** -0.5, 0.109375, ((0, 16), (1, 2)))
    routes_keys = jax.random.split(jax.random.fold_in(seeds[15], 1), TOKENS // SEQ_DEV)
    routes_turns = jax.random.permutation(jax.random.fold_in(seeds[15], 3), TOKENS // SEQ_DEV)
    routes = jax.vmap(lambda own, number: shared_out(jax.random.fold_in(seeds[15], 2), own, number, SEQ_DEV, EXPERTS, TOPK, CAP, 1))(routes_keys, routes_turns).reshape((TOKENS, TOPK))
    route_w = jnp.clip(0.099609375 + 0.9003906 * jax.random.uniform(seeds[16], (TOKENS, TOPK), jnp.float32) ** levels(seeds[16], (TOKENS, TOPK), ((0, 16),), -0.2, 0.2), 0.099609375, 1.0).astype(jnp.bfloat16)
    return dict(tokens=tokens, state=state, norm_mix=norm_mix, w_query=w_query, w_key=w_key, w_value=w_value, w_out=w_out, norm_ffn=norm_ffn, gate_vector=gate_vector, dense_gate=dense_gate, dense_up=dense_up, dense_down=dense_down, exp_gate=exp_gate, exp_up=exp_up, exp_down=exp_down, routes=routes, route_w=route_w)


epsilon = 1e-06

def reference(tokens, state, norm_mix, w_query, w_key, w_value, w_out, norm_ffn, gate_vector, dense_gate, dense_up, dense_down, exp_gate, exp_up, exp_down, routes, route_w):
    highest = lax.Precision.HIGHEST
    tok_f = tokens.astype(jnp.float32)
    normed = (tok_f * lax.rsqrt(lax.optimization_barrier(jnp.mean(tok_f * tok_f, axis=1, keepdims=True)) + epsilon) * norm_mix).astype(jnp.bfloat16)
    query = jnp.dot(normed, w_query, preferred_element_type=jnp.float32).astype(jnp.bfloat16)
    key_rows = jnp.dot(normed, w_key, preferred_element_type=jnp.float32).astype(jnp.bfloat16)
    value_rows = jnp.dot(normed, w_value, preferred_element_type=jnp.float32).astype(jnp.bfloat16)
    row_count = tokens.shape[0]
    query3 = query.astype(jnp.float32).reshape(row_count, HEADS, HEAD)
    key3 = key_rows.astype(jnp.float32).reshape(row_count, HEADS, HEAD) * HEAD ** (-0.5)
    value3 = value_rows.astype(jnp.float32).reshape(row_count, HEADS, HEAD)
    head_ids = jnp.arange(HEADS, dtype=jnp.float32)
    decay = 1.0 - jnp.exp2(-3.0 - 2.0 * head_ids)
    new_state = decay[None, :, None, None] * state + jnp.einsum('shd,she->shde', key3, value3, precision=highest)
    read = jnp.einsum('shd,shde->she', query3, new_state, precision=highest)
    centre = lax.optimization_barrier(jnp.mean(read, axis=2, keepdims=True))
    spread = lax.optimization_barrier(jnp.mean(jnp.square(read - centre), axis=2, keepdims=True))
    heads_out = ((read - centre) * lax.rsqrt(spread + epsilon)).astype(jnp.bfloat16).reshape(row_count, HEADS * HEAD)
    group_cols = HEADS * HEAD // N_TP
    mix_sum = jnp.zeros((row_count, D), jnp.float32)
    for group in range(N_TP):
        lower = group * group_cols
        partial_value = jnp.dot(heads_out[:, lower:lower + group_cols], w_out[lower:lower + group_cols], preferred_element_type=jnp.float32)
        rounded = lax.optimization_barrier(partial_value.astype(jnp.bfloat16))
        mix_sum = mix_sum + rounded.astype(jnp.float32)
    after = (tok_f + mix_sum).astype(jnp.bfloat16)
    after_f = after.astype(jnp.float32)
    normed2 = (after_f * lax.rsqrt(lax.optimization_barrier(jnp.mean(after_f * after_f, axis=1, keepdims=True)) + epsilon) * norm_ffn).astype(jnp.bfloat16)
    dense_pre = jnp.dot(normed2, dense_gate, preferred_element_type=jnp.float32)
    up_pre = jnp.dot(normed2, dense_up, preferred_element_type=jnp.float32)
    logit = jnp.dot(normed2, gate_vector, preferred_element_type=jnp.float32)
    dense_hidden = (jax.nn.sigmoid(logit)[:, None] * jax.nn.silu(dense_pre) * up_pre).astype(jnp.bfloat16)
    dense = jnp.dot(dense_hidden, dense_down, preferred_element_type=jnp.float32)
    group_size = N_EP // EXPERTS
    part_ff = exp_gate.shape[2]
    gate_all = exp_gate.reshape(EXPERTS, group_size, D, part_ff).transpose(0, 2, 1, 3).reshape(EXPERTS, D, group_size * part_ff)
    up_all = exp_up.reshape(EXPERTS, group_size, D, part_ff).transpose(0, 2, 1, 3).reshape(EXPERTS, D, group_size * part_ff)
    down_all = exp_down.reshape(EXPERTS, group_size * part_ff, D)
    onehot = (routes[:, :, None] == jnp.arange(EXPERTS, dtype=jnp.int32)[None, None, :]).astype(jnp.float32)
    member = lax.optimization_barrier(jnp.sum(onehot, axis=1))
    weight = lax.optimization_barrier(jnp.sum(onehot * route_w.astype(jnp.float32)[:, :, None], axis=1))
    member_b = member.reshape(N_EP, SEQ_DEV, EXPERTS)
    slot_b = jnp.cumsum(member_b, axis=1) - member_b
    weight_b = weight.reshape(N_EP, SEQ_DEV, EXPERTS)
    rows_b = normed2.astype(jnp.float32).reshape(N_EP, SEQ_DEV, D)
    slot_ids = jnp.arange(CAP, dtype=jnp.float32)

    def one_expert(total, inputs):
        gate_w, up_w, down_w, pick, place, scale = inputs
        select = pick[:, None, :] * (place[:, None, :] == slot_ids[None, :, None]).astype(jnp.float32)
        chosen = jnp.einsum('ncr,nrd->ncd', select, rows_b, precision=highest).astype(jnp.bfloat16).reshape(N_EP * CAP, D)
        gate_pre = jnp.dot(chosen, gate_w, preferred_element_type=jnp.float32)
        up_part = jnp.dot(chosen, up_w, preferred_element_type=jnp.float32)
        hidden = (jax.nn.silu(gate_pre) * up_part).astype(jnp.bfloat16)
        result = jnp.dot(hidden, down_w, preferred_element_type=jnp.float32).reshape(N_EP, CAP, D)
        contrib = jnp.einsum('ncr,ncd->nrd', select * scale[:, None, :], result, precision=highest)
        return (total + contrib, None)
    moe, _ = lax.scan(one_expert, jnp.zeros((N_EP, SEQ_DEV, D), jnp.float32), (gate_all, up_all, down_all, member_b.transpose(2, 0, 1), slot_b.transpose(2, 0, 1), weight_b.transpose(2, 0, 1)))
    mixed = (after_f + moe.reshape(row_count, D) + dense).astype(jnp.bfloat16)
    return (mixed, new_state)
```

```python
import functools

import jax
import jax.numpy as jnp
from jax import lax
from jax.experimental import pallas as pl
from jax.experimental.pallas import tpu as pltpu
from jax.sharding import PartitionSpec as P

EXPERTS = 8
epsilon = 1e-06
MESH = pl.DeviceIdType.MESH
F32 = jnp.float32
BF16 = jnp.bfloat16


def dot(a, b):
    return jnp.dot(a, b, preferred_element_type=F32)


def silu(v):
    return v / (1.0 + jnp.exp(-v))


def kernel(
    A,
    B,
    tokens,
    norm_mix,
    routes,
    route_w,
    extra,
    state,
    w_query,
    w_key,
    w_value,
    w_out,
    dense_gate,
    dense_up,
    dense_down,
    exp_gate,
    exp_up,
    exp_down,
    mixed,
    new_state,
    tok_p,
    ext_p,
    wq,
    wk,
    wv,
    wo_o,
    wo_p,
    dg,
    du,
    dd,
    eg,
    eu,
    ed,
    st,
    ns,
    ho_o,
    ho_p,
    aux,
    xo,
    xp,
    y0,
    yx_s,
    yx_r,
    ys,
    rsx,
    zs,
    rsz,
    lsem,
    psem_s,
    psem_r,
    axz_s,
    axz_r,
    axx_s,
    axx_r,
    gz_s,
    gz_r,
    gx_s,
    gx_r,
    gp_s,
    gp_r,
    yx_ss,
    yx_rs,
    rx_s,
    rx_r,
    rz_s,
    rz_r,
):
    R, H = tokens.shape
    D = 2 * H
    heads, hs = state.shape[1], state.shape[2]
    HW = heads * hs
    n = A * B
    me = lax.axis_index("ep")
    tp = lax.axis_index("tp")
    z, xy = me // B, me % B
    other = 1 - tp
    expert = me // (n // EXPERTS)
    partner = {"ep": me, "tp": other}
    xpeer = [{"ep": z * B + (xy + j) % B, "tp": tp} for j in range(B)]
    zpeer = [{"ep": ((z + i) % A) * B + xy, "tp": tp} for i in range(A)]

    own_at = pl.multiple_of(tp * H, H)
    oth_at = pl.multiple_of(other * H, H)
    own, oth = pl.ds(own_at, H), pl.ds(oth_at, H)

    sent = []

    def remote(src, dst, s, r, dev):
        copy = pltpu.make_async_remote_copy(
            src_ref=src, dst_ref=dst, send_sem=s, recv_sem=r, device_id=dev, device_id_type=MESH
        )
        copy.start()
        sent.append(copy)
        return copy

    local = {}

    def load(name, k, src, dst):
        copy = pltpu.make_async_copy(src, dst, lsem.at[k])
        copy.start()
        local[name] = copy

    barrier = pltpu.get_barrier_semaphore()
    for dev in [partner] + xpeer[1:] + zpeer[1:]:
        pl.semaphore_signal(barrier, inc=1, device_id=dev, device_id_type=MESH)

    for t, (src, dst) in enumerate(((w_query, wq), (w_key, wk), (w_value, wv))):
        load(f"p{t}o", 2 * t, src.at[own, :], dst.at[0])
        load(f"p{t}p", 2 * t + 1, src.at[oth, :], dst.at[1])
    load("st", 6, state, st)
    load("wo0", 7, w_out.at[:, own], wo_o.at[0])
    load("wo1", 8, w_out.at[:, oth], wo_o.at[1])
    load("dg", 9, dense_gate, dg.at[0])
    load("du", 10, dense_up, du.at[0])
    load("dd", 11, dense_down, dd)
    load("eg0", 12, exp_gate.at[0, own, :], eg.at[0])
    load("eu0", 13, exp_up.at[0, own, :], eu.at[0])
    load("eg1", 14, exp_gate.at[0, oth, :], eg.at[1])
    load("eu1", 15, exp_up.at[0, oth, :], eu.at[1])
    load("ed1", 16, exp_down.at[0, :, oth], ed.at[1])
    load("ed0", 17, exp_down.at[0, :, own], ed.at[0])

    lane = lax.broadcasted_iota(jnp.int32, (R, 128), 1)
    wt = jnp.zeros((R, 128), F32)
    for t in range(routes.shape[1]):
        wt = wt + jnp.where(lane == routes[:, t : t + 1], route_w[:, t : t + 1].astype(F32), 0.0)
    aux[0, 0] = wt.astype(BF16)

    pl.semaphore_wait(barrier, 1 + (B - 1) + (A - 1))

    c_tok = remote(tokens, tok_p, psem_s.at[0], psem_r.at[0], partner)
    c_ext = remote(extra, ext_p, psem_s.at[1], psem_r.at[1], partner)
    c_wo0 = remote(w_out.at[:, oth], wo_p.at[0], psem_s.at[2], psem_r.at[2], partner)
    c_wo1 = remote(w_out.at[:, own], wo_p.at[1], psem_s.at[3], psem_r.at[3], partner)
    c_dg = remote(dense_gate, dg.at[1], psem_s.at[4], psem_r.at[4], partner)
    c_du = remote(dense_up, du.at[1], psem_s.at[5], psem_r.at[5], partner)
    c_axz = [None] + [
        remote(aux.at[0, 0], aux.at[0, A - i], axz_s.at[i], axz_r.at[A - i], zpeer[i])
        for i in range(1, A)
    ]

    tok_f = tokens[...].astype(F32)
    c_tok.wait_recv()
    tok_pf = tok_p[...].astype(F32)
    total = jnp.sum(tok_f * tok_f, axis=1, keepdims=True) + jnp.sum(
        tok_pf * tok_pf, axis=1, keepdims=True
    )
    scale = lax.rsqrt(total / D + epsilon)
    gain_o = norm_mix[:, own]
    gain_p = norm_mix[:, oth]
    nx_o = (tok_f * scale * gain_o).astype(BF16)
    nx_p = (tok_pf * scale * gain_p).astype(BF16)
    proj = []
    for t, w in enumerate((wq, wk, wv)):
        local[f"p{t}o"].wait()
        part = dot(nx_o, w[0])
        local[f"p{t}p"].wait()
        proj.append((part + dot(nx_p, w[1])).astype(BF16).astype(F32))
    q, k, v = proj
    k = k * hs ** (-0.5)
    pad = jnp.zeros((128 - R, HW), F32)
    q_t = jnp.concatenate([q, pad], axis=0).T
    k_t = jnp.concatenate([k, pad], axis=0).T
    head_id = tp * heads
    local["st"].wait()
    decays = []
    for h in range(heads):
        cols = slice(h * hs, (h + 1) * hs)
        idv = jnp.zeros((1, 128), F32) + (head_id + h).astype(F32)
        decay = 1.0 - jnp.exp2(-3.0 - 2.0 * idv)
        decays.append(decay)
        rows = []
        for s in range(R):
            rows.append(jnp.sum(st[s, h] * q_t[cols, s : s + 1], axis=0, keepdims=True))
        qs = jnp.concatenate(rows, axis=0)
        qk = jnp.sum(q[:, cols] * k[:, cols], axis=1, keepdims=True)
        read = decay * qs + qk * v[:, cols]
        centre = jnp.mean(read, axis=1, keepdims=True)
        dev = read - centre
        spread = jnp.mean(dev * dev, axis=1, keepdims=True)
        ho_o[:, cols] = (dev * lax.rsqrt(spread + epsilon)).astype(BF16)
    c_ho = remote(ho_o, ho_p, psem_s.at[6], psem_r.at[6], partner)
    ho = ho_o[...]
    local["wo0"].wait()
    local["wo1"].wait()
    a_o = dot(ho, wo_o[0]).astype(BF16).astype(F32)
    a_p = dot(ho, wo_o[1]).astype(BF16).astype(F32)
    c_wo0.wait_recv()
    c_wo1.wait_recv()
    c_ho.wait_recv()
    hp = ho_p[...]
    a_o = a_o + dot(hp, wo_p[0]).astype(BF16).astype(F32)
    a_p = a_p + dot(hp, wo_p[1]).astype(BF16).astype(F32)
    after = (tok_f + a_o).astype(BF16).astype(F32)
    after_p = (tok_pf + a_p).astype(BF16).astype(F32)
    squares = jnp.sum(after * after, axis=1, keepdims=True) + jnp.sum(
        after_p * after_p, axis=1, keepdims=True
    )
    xo[0, 0] = (after * lax.rsqrt(squares / D + epsilon) * extra[0:1, :]).astype(BF16)

    c_gz = [None] * A
    c_gx = {}
    c_gp = {}
    for i in range(1, A):
        c_gz[i] = remote(xo.at[0, 0], xo.at[0, A - i], gz_s.at[i], gz_r.at[A - i], zpeer[i])

    def spread_block(i):
        for j in range(1, B):
            c_gx[j, i] = remote(
                xo.at[0, i],
                xo.at[B - j, i],
                gx_s.at[j, i],
                gx_r.at[B - j, i],
                xpeer[j],
            )

    def to_partner(j, i):
        c_gp[j, i] = remote(
            xo.at[j, i], xp.at[j, i], gp_s.at[j, i], gp_r.at[j, i], partner
        )

    spread_block(0)
    to_partner(0, 0)
    for i in range(1, A):
        c_axz[A - i].wait_recv()
    c_axx = [None] + [
        remote(aux.at[0], aux.at[B - j], axx_s.at[j], axx_r.at[B - j], xpeer[j])
        for j in range(1, B)
    ]
    order = sorted(range(1, A), key=lambda i: min(i, A - i))
    for i in order:
        c_gz[A - i].wait_recv()
        spread_block(i)
        to_partner(0, i)

    for h in range(heads):
        cols = slice(h * hs, (h + 1) * hs)
        for s in range(R):
            ns[s, h] = decays[h] * st[s, h] + k_t[cols, s : s + 1] * v[s : s + 1, cols]
    c_ns = pltpu.make_async_copy(ns, new_state, lsem.at[18])
    c_ns.start()

    c_ext.wait_recv()
    for name in ("dg", "du", "dd", "eg0", "eu0", "eg1", "eu1", "ed1", "ed0"):
        local[name].wait()
    c_dg.wait_recv()
    c_du.wait_recv()

    AR = A * R

    def ffn(j0, nj, slot):
        rows = nj * AR
        x_o = xo[j0 : j0 + nj].reshape(rows, H)
        gate = dot(x_o, eg[0])
        up = dot(x_o, eu[0])
        d_gate = dot(x_o, dg[0])
        d_up = dot(x_o, du[0])
        logit = jnp.sum(x_o.astype(F32) * extra[1:2, :], axis=1, keepdims=True)
        for j in range(j0, j0 + nj):
            for i in range(A):
                c_gp[j, i].wait_recv()
        x_p = xp[j0 : j0 + nj].reshape(rows, H)
        gate = gate + dot(x_p, eg[1])
        up = up + dot(x_p, eu[1])
        d_gate = d_gate + dot(x_p, dg[1])
        d_up = d_up + dot(x_p, du[1])
        logit = logit + jnp.sum(x_p.astype(F32) * ext_p[1:2, :], axis=1, keepdims=True)
        lanes = lax.broadcasted_iota(jnp.int32, (rows, 128), 1)
        table = aux[j0 : j0 + nj].reshape(rows, 128).astype(F32)
        weight = jnp.sum(jnp.where(lanes == expert, table, 0.0), axis=1, keepdims=True)
        hidden = (silu(gate) * up).astype(BF16)
        d_hidden = (1.0 / (1.0 + jnp.exp(-logit)) * silu(d_gate) * d_up).astype(BF16)
        yx_s[j0 : j0 + nj] = (weight * dot(hidden, ed[1])).astype(BF16).reshape(nj, A, R, H)
        c_yx = remote(
            yx_s.at[pl.ds(j0, nj)],
            yx_r.at[pl.ds(j0, nj)],
            yx_ss.at[slot],
            yx_rs.at[slot],
            partner,
        )
        y = weight * dot(hidden, ed[0]) + dot(d_hidden, dd[...])
        c_yx.wait_recv()
        return y.reshape(nj, A, R, H) + yx_r[j0 : j0 + nj].astype(F32)

    y0[...] = ffn(0, 1, 0)[0]

    for i in [0] + order:
        for j in range(1, B):
            c_gx[B - j, i].wait_recv()
            to_partner(j, i)
    for j in range(1, B):
        c_axx[B - j].wait_recv()
    group = max(g for g in range(1, B) if (B - 1) % g == 0 and (g * AR <= 256 or g == 1))
    c_rx = [None] * B
    for slot, j0 in enumerate(range(1, B, group)):
        y = ffn(j0, group, slot + 1)
        ys[j0 : j0 + group] = y.astype(BF16)
        for j in range(j0, j0 + group):
            c_rx[j] = remote(ys.at[j], rsx.at[B - j], rx_s.at[j], rx_r.at[B - j], xpeer[j])

    total = y0[...]
    for j in range(1, B):
        c_rx[B - j].wait_recv()
        total = total + rsx[j].astype(F32)
    zs[...] = total.astype(BF16)
    c_rz = [None] + [
        remote(zs.at[i], rsz.at[A - i], rz_s.at[i], rz_r.at[A - i], zpeer[i])
        for i in range(1, A)
    ]
    result = after + total[0]
    for i in range(1, A):
        c_rz[A - i].wait_recv()
        result = result + rsz[i].astype(F32)
    mixed[...] = result.astype(BF16)
    for copy in sent:
        copy.wait_send()
    c_ns.wait()


def body(
    tokens,
    state,
    norm_mix,
    w_query,
    w_key,
    w_value,
    w_out,
    norm_ffn,
    gate_vector,
    dense_gate,
    dense_up,
    dense_down,
    exp_gate,
    exp_up,
    exp_down,
    routes,
    route_w,
):
    n = lax.axis_size("ep")
    A = 1
    while (2 * A) * (2 * A) <= n:
        A = 2 * A
    B = n // A
    R, H = tokens.shape
    heads, hs = state.shape[1], state.shape[2]
    HW = heads * hs
    FE = exp_gate.shape[2]
    FD = dense_gate.shape[1]
    extra = jnp.stack([norm_ffn, gate_vector.astype(F32)])
    vm = pl.BlockSpec(memory_space=pltpu.VMEM)
    hbm = pl.BlockSpec(memory_space=pl.ANY)
    V = pltpu.VMEM
    sem = lambda *shape: pltpu.SemaphoreType.DMA(shape)
    return pl.pallas_call(
        functools.partial(kernel, A, B),
        out_shape=(
            jax.ShapeDtypeStruct((R, H), BF16),
            jax.ShapeDtypeStruct(state.shape, F32),
        ),
        in_specs=[vm] * 5 + [hbm] * 11,
        out_specs=(vm, hbm),
        scratch_shapes=[
            V((R, H), BF16),
            V((2, H), F32),
            V((2, H, HW), BF16),
            V((2, H, HW), BF16),
            V((2, H, HW), BF16),
            V((2, HW, H), BF16),
            V((2, HW, H), BF16),
            V((2, H, FD), BF16),
            V((2, H, FD), BF16),
            V((FD, H), BF16),
            V((2, H, FE), BF16),
            V((2, H, FE), BF16),
            V((2, FE, H), BF16),
            V(state.shape, F32),
            V(state.shape, F32),
            V((R, HW), BF16),
            V((R, HW), BF16),
            V((B, A, R, 128), BF16),
            V((B, A, R, H), BF16),
            V((B, A, R, H), BF16),
            V((A, R, H), F32),
            V((B, A, R, H), BF16),
            V((B, A, R, H), BF16),
            V((B, A, R, H), BF16),
            V((B, A, R, H), BF16),
            V((A, R, H), BF16),
            V((A, R, H), BF16),
            sem(19),
            sem(7),
            sem(7),
            sem(A),
            sem(A),
            sem(B),
            sem(B),
            sem(A),
            sem(A),
            sem(B, A),
            sem(B, A),
            sem(B, A),
            sem(B, A),
            sem(B),
            sem(B),
            sem(B),
            sem(B),
            sem(A),
            sem(A),
        ],
        compiler_params=pltpu.CompilerParams(
            collective_id=0, has_side_effects=True, vmem_limit_bytes=67043328
        ),
        name="layer",
    )(
        tokens,
        norm_mix.reshape(1, -1),
        routes,
        route_w,
        extra,
        state,
        w_query,
        w_key,
        w_value,
        w_out,
        dense_gate,
        dense_up,
        dense_down,
        exp_gate,
        exp_up,
        exp_down,
    )


def solution(mesh):
    return jax.shard_map(
        body,
        mesh=mesh,
        in_specs=(
            P("ep", "tp"),
            P("ep", "tp", None, None),
            P(),
            P(None, "tp"),
            P(None, "tp"),
            P(None, "tp"),
            P("tp", None),
            P("tp"),
            P("tp"),
            P("tp", "ep"),
            P("tp", "ep"),
            P("ep", "tp"),
            P("ep", None, "tp"),
            P("ep", None, "tp"),
            P("ep", "tp", None),
            P("ep", None),
            P("ep", None),
        ),
        out_specs=(P("ep", "tp"), P("ep", "tp", None, None)),
        check_vma=False,
    )
```

```python
import functools

import jax
import jax.numpy as jnp
from jax import lax
from jax.experimental import pallas as pl
from jax.experimental.pallas import tpu as pltpu
from jax.sharding import PartitionSpec as P

EXPERTS = 8
epsilon = 1e-06
MESH = pl.DeviceIdType.MESH
F32 = jnp.float32
BF16 = jnp.bfloat16


def dot(a, b):
    return jnp.dot(a, b, preferred_element_type=F32)


def dot_t(a, b):
    return lax.dot_general(a, b, (((1,), (1,)), ((), ())), preferred_element_type=F32)


def silu(v):
    return v / (1.0 + jnp.exp(-v))


def kernel(
    A,
    B,
    tokens_h,
    norm_mix_h,
    routes_h,
    route_w_h,
    norm_ffn_h,
    gate_vec_h,
    state,
    w_query,
    w_key,
    w_value,
    w_out,
    dense_gate,
    dense_up,
    dense_down,
    exp_gate,
    exp_up,
    exp_down,
    mixed,
    ns,
    tokens,
    norm_mix,
    routes,
    route_w,
    norm_ffn,
    gate_vec,
    tok_p,
    gvec_p,
    wq,
    wk,
    wv,
    wo_o,
    wo_p,
    dg,
    du,
    dd,
    eg,
    eu,
    ed,
    st,
    ho_o,
    ho_p,
    aux,
    xo,
    xp,
    y0,
    yx_s,
    yx_r,
    ys,
    rsx,
    zs,
    rsz,
    lsem,
    psem_s,
    psem_r,
    axz_s,
    axz_r,
    axx_s,
    axx_r,
    gz_s,
    gz_r,
    gx_s,
    gx_r,
    gp_s,
    gp_r,
    yx_ss,
    yx_rs,
    rx_s,
    rx_r,
    rz_s,
    rz_r,
):
    R, H = tokens.shape
    D = 2 * H
    heads, hs = state.shape[1], state.shape[2]
    HW = heads * hs
    n = A * B
    me = lax.axis_index("ep")
    tp = lax.axis_index("tp")
    z, xy = me // B, me % B
    other = 1 - tp
    expert = me // (n // EXPERTS)
    partner = {"ep": me, "tp": other}
    xpeer = [{"ep": z * B + (xy + j) % B, "tp": tp} for j in range(B)]
    zpeer = [{"ep": ((z + i) % A) * B + xy, "tp": tp} for i in range(A)]

    own_at = pl.multiple_of(tp * H, H)
    oth_at = pl.multiple_of(other * H, H)
    own, oth = pl.ds(own_at, H), pl.ds(oth_at, H)

    sent = []

    def remote(src, dst, s, r, dev):
        copy = pltpu.make_async_remote_copy(
            src_ref=src, dst_ref=dst, send_sem=s, recv_sem=r, device_id=dev, device_id_type=MESH
        )
        copy.start()
        sent.append(copy)
        return copy

    local = {}

    def load(name, k, src, dst):
        copy = pltpu.make_async_copy(src, dst, lsem.at[k])
        copy.start()
        local[name] = copy

    small = (
        (tokens_h, tokens),
        (norm_mix_h, norm_mix),
        (routes_h, routes),
        (route_w_h, route_w),
        (norm_ffn_h, norm_ffn),
        (gate_vec_h, gate_vec),
    )
    barrier = pltpu.get_barrier_semaphore()
    for dev in [partner] + xpeer[1:] + zpeer[1:]:
        pl.semaphore_signal(barrier, inc=1, device_id=dev, device_id_type=MESH)

    for t, (src, dst) in enumerate(small):
        load(f"s{t}", 19 + t, src, dst)
    for t, (src, dst) in enumerate(((w_query, wq), (w_key, wk), (w_value, wv))):
        load(f"p{t}o", 2 * t, src.at[own, :], dst.at[0])
        load(f"p{t}p", 2 * t + 1, src.at[oth, :], dst.at[1])
    load("st", 6, state, st)
    load("wo0", 7, w_out.at[:, own], wo_o.at[0])
    load("wo1", 8, w_out.at[:, oth], wo_o.at[1])
    load("dg", 9, dense_gate, dg.at[0])
    load("du", 10, dense_up, du.at[0])
    load("dd", 11, dense_down, dd)
    load("eg0", 12, exp_gate.at[:, own], eg.at[0])
    load("eu0", 13, exp_up.at[:, own], eu.at[0])
    load("eg1", 14, exp_gate.at[:, oth], eg.at[1])
    load("eu1", 15, exp_up.at[:, oth], eu.at[1])
    load("ed1", 16, exp_down.at[0, :, oth], ed.at[1])
    load("ed0", 17, exp_down.at[0, :, own], ed.at[0])

    for t in (2, 3):
        local[f"s{t}"].wait()
    row_id = lax.broadcasted_iota(jnp.int32, (EXPERTS, R), 0)
    wt = jnp.zeros((EXPERTS, R), F32)
    named = routes[...]
    gains = route_w[...].astype(F32)
    for t in range(routes.shape[0]):
        wt = wt + jnp.where(row_id == named[t : t + 1, :], gains[t : t + 1, :], 0.0)
    wt = jnp.concatenate([wt, jnp.zeros((EXPERTS, 128 - R), F32)], axis=1)
    wt = jnp.concatenate([wt, jnp.zeros((128 - EXPERTS, 128), F32)], axis=0)
    aux[0, 0] = wt.T[:R].astype(BF16)

    for t in (0, 1, 4, 5):
        local[f"s{t}"].wait()
    pl.semaphore_wait(barrier, 1 + (B - 1) + (A - 1))

    c_tok = remote(tokens, tok_p, psem_s.at[0], psem_r.at[0], partner)
    c_ext = remote(gate_vec, gvec_p, psem_s.at[1], psem_r.at[1], partner)
    c_wo0 = remote(w_out.at[:, oth], wo_p.at[0], psem_s.at[2], psem_r.at[2], partner)
    c_wo1 = remote(w_out.at[:, own], wo_p.at[1], psem_s.at[3], psem_r.at[3], partner)
    c_dg = remote(dense_gate, dg.at[1], psem_s.at[4], psem_r.at[4], partner)
    c_du = remote(dense_up, du.at[1], psem_s.at[5], psem_r.at[5], partner)
    c_axz = [None] + [
        remote(aux.at[0, 0], aux.at[0, A - i], axz_s.at[i], axz_r.at[A - i], zpeer[i])
        for i in range(1, A)
    ]

    tok_f = tokens[...].astype(F32)
    c_tok.wait_recv()
    tok_pf = tok_p[...].astype(F32)
    total = jnp.sum(tok_f * tok_f, axis=1, keepdims=True) + jnp.sum(
        tok_pf * tok_pf, axis=1, keepdims=True
    )
    scale = lax.rsqrt(total / D + epsilon)
    gain_o = norm_mix[:, own]
    gain_p = norm_mix[:, oth]
    nx_o = (tok_f * scale * gain_o).astype(BF16)
    nx_p = (tok_pf * scale * gain_p).astype(BF16)
    proj = []
    for t, w in enumerate((wq, wk, wv)):
        local[f"p{t}o"].wait()
        part = dot(nx_o, w[0])
        local[f"p{t}p"].wait()
        proj.append((part + dot(nx_p, w[1])).astype(BF16).astype(F32))
    q, k, v = proj
    k = k * hs ** (-0.5)
    pad = jnp.zeros((128 - R, HW), F32)
    q_t = jnp.concatenate([q, pad], axis=0).T
    k_t = jnp.concatenate([k, pad], axis=0).T
    head_id = tp * heads
    local["st"].wait()
    decays = []
    for h in range(heads):
        cols = slice(h * hs, (h + 1) * hs)
        idv = jnp.zeros((1, 128), F32) + (head_id + h).astype(F32)
        decay = 1.0 - jnp.exp2(-3.0 - 2.0 * idv)
        decays.append(decay)
        rows = []
        for s in range(R):
            rows.append(jnp.sum(st[s, h] * q_t[cols, s : s + 1], axis=0, keepdims=True))
        qs = jnp.concatenate(rows, axis=0)
        qk = jnp.sum(q[:, cols] * k[:, cols], axis=1, keepdims=True)
        read = decay * qs + qk * v[:, cols]
        centre = jnp.mean(read, axis=1, keepdims=True)
        dev = read - centre
        spread = jnp.mean(dev * dev, axis=1, keepdims=True)
        ho_o[:, cols] = (dev * lax.rsqrt(spread + epsilon)).astype(BF16)
    c_ho = remote(ho_o, ho_p, psem_s.at[6], psem_r.at[6], partner)
    ho = ho_o[...]
    local["wo0"].wait()
    local["wo1"].wait()
    a_o = dot(ho, wo_o[0]).astype(BF16).astype(F32)
    a_p = dot(ho, wo_o[1]).astype(BF16).astype(F32)
    c_wo0.wait_recv()
    c_wo1.wait_recv()
    c_ho.wait_recv()
    hp = ho_p[...]
    a_o = a_o + dot(hp, wo_p[0]).astype(BF16).astype(F32)
    a_p = a_p + dot(hp, wo_p[1]).astype(BF16).astype(F32)
    after = (tok_f + a_o).astype(BF16).astype(F32)
    after_p = (tok_pf + a_p).astype(BF16).astype(F32)
    squares = jnp.sum(after * after, axis=1, keepdims=True) + jnp.sum(
        after_p * after_p, axis=1, keepdims=True
    )
    xo[0, 0] = (after * lax.rsqrt(squares / D + epsilon) * norm_ffn[...]).astype(BF16)

    c_gz = [None] * A
    c_gx = {}
    c_gp = {}
    for i in range(1, A):
        c_gz[i] = remote(xo.at[0, 0], xo.at[0, A - i], gz_s.at[i], gz_r.at[A - i], zpeer[i])

    def spread_block(i):
        for j in range(1, B):
            c_gx[j, i] = remote(
                xo.at[0, i],
                xo.at[B - j, i],
                gx_s.at[j, i],
                gx_r.at[B - j, i],
                xpeer[j],
            )

    def to_partner(j, i):
        c_gp[j, i] = remote(
            xo.at[j, i], xp.at[j, i], gp_s.at[j, i], gp_r.at[j, i], partner
        )

    spread_block(0)
    to_partner(0, 0)
    for i in range(1, A):
        c_axz[A - i].wait_recv()
    c_axx = [None] + [
        remote(aux.at[0], aux.at[B - j], axx_s.at[j], axx_r.at[B - j], xpeer[j])
        for j in range(1, B)
    ]
    order = sorted(range(1, A), key=lambda i: min(i, A - i))
    for i in order:
        c_gz[A - i].wait_recv()
        spread_block(i)
        to_partner(0, i)

    for h in range(heads):
        cols = slice(h * hs, (h + 1) * hs)
        for s in range(R):
            ns[s, h] = decays[h] * st[s, h] + k_t[cols, s : s + 1] * v[s : s + 1, cols]

    c_ext.wait_recv()
    for name in ("dg", "du", "dd", "eg0", "eu0", "eg1", "eu1", "ed1", "ed0"):
        local[name].wait()
    c_dg.wait_recv()
    c_du.wait_recv()

    AR = A * R

    def gate_row(ref):
        part = ref[...].astype(F32)
        return jnp.concatenate([part[r : r + 1] for r in range(H // 128)], axis=1)

    gvec_o = gate_row(gate_vec)
    gvec_q = gate_row(gvec_p)

    def ffn(j0, nj, slot):
        rows = nj * AR
        x_o = xo[j0 : j0 + nj].reshape(rows, H)
        gate = dot_t(x_o, eg[0])
        up = dot_t(x_o, eu[0])
        d_gate = dot_t(x_o, dg[0])
        d_up = dot_t(x_o, du[0])
        logit = jnp.sum(x_o.astype(F32) * gvec_o, axis=1, keepdims=True)
        for j in range(j0, j0 + nj):
            for i in range(A):
                c_gp[j, i].wait_recv()
        x_p = xp[j0 : j0 + nj].reshape(rows, H)
        gate = gate + dot_t(x_p, eg[1])
        up = up + dot_t(x_p, eu[1])
        d_gate = d_gate + dot_t(x_p, dg[1])
        d_up = d_up + dot_t(x_p, du[1])
        logit = logit + jnp.sum(x_p.astype(F32) * gvec_q, axis=1, keepdims=True)
        lanes = lax.broadcasted_iota(jnp.int32, (rows, 128), 1)
        table = aux[j0 : j0 + nj].reshape(rows, 128).astype(F32)
        weight = jnp.sum(jnp.where(lanes == expert, table, 0.0), axis=1, keepdims=True)
        hidden = (silu(gate) * up).astype(BF16)
        d_hidden = (1.0 / (1.0 + jnp.exp(-logit)) * silu(d_gate) * d_up).astype(BF16)
        yx_s[j0 : j0 + nj] = (weight * dot(hidden, ed[1])).astype(BF16).reshape(nj, A, R, H)
        c_yx = remote(
            yx_s.at[pl.ds(j0, nj)],
            yx_r.at[pl.ds(j0, nj)],
            yx_ss.at[slot],
            yx_rs.at[slot],
            partner,
        )
        y = weight * dot(hidden, ed[0]) + dot(d_hidden, dd[...])
        c_yx.wait_recv()
        return y.reshape(nj, A, R, H) + yx_r[j0 : j0 + nj].astype(F32)

    y0[...] = ffn(0, 1, 0)[0]

    for i in [0] + order:
        for j in range(1, B):
            c_gx[B - j, i].wait_recv()
            to_partner(j, i)
    for j in range(1, B):
        c_axx[B - j].wait_recv()
    group = max(g for g in range(1, B) if (B - 1) % g == 0 and (g * AR <= 256 or g == 1))
    c_rx = [None] * B
    for slot, j0 in enumerate(range(1, B, group)):
        y = ffn(j0, group, slot + 1)
        ys[j0 : j0 + group] = y.astype(BF16)
        for j in range(j0, j0 + group):
            c_rx[j] = remote(ys.at[j], rsx.at[B - j], rx_s.at[j], rx_r.at[B - j], xpeer[j])

    total = y0[...]
    for j in range(1, B):
        c_rx[B - j].wait_recv()
        total = total + rsx[j].astype(F32)
    zs[...] = total.astype(BF16)
    c_rz = [None] + [
        remote(zs.at[i], rsz.at[A - i], rz_s.at[i], rz_r.at[A - i], zpeer[i])
        for i in range(1, A)
    ]
    result = after + total[0]
    for i in range(1, A):
        c_rz[A - i].wait_recv()
        result = result + rsz[i].astype(F32)
    mixed[...] = result.astype(BF16)
    for copy in sent:
        copy.wait_send()


def store(a_in, b_in, a_out, b_out, sems):
    first = pltpu.make_async_copy(b_in, b_out, sems.at[0])
    second = pltpu.make_async_copy(a_in, a_out, sems.at[1])
    first.start()
    second.start()
    first.wait()
    second.wait()


def body(
    tokens,
    state,
    norm_mix,
    w_query,
    w_key,
    w_value,
    w_out,
    norm_ffn,
    gate_vector,
    dense_gate,
    dense_up,
    dense_down,
    exp_gate,
    exp_up,
    exp_down,
    routes,
    route_w,
):
    n = lax.axis_size("ep")
    A = 1
    while (2 * A) * (2 * A) <= n:
        A = 2 * A
    B = n // A
    R, H = tokens.shape
    heads, hs = state.shape[1], state.shape[2]
    HW = heads * hs
    FE = exp_gate.shape[2]
    FD = dense_gate.shape[1]
    vm = pl.BlockSpec(memory_space=pltpu.VMEM)
    hbm = pl.BlockSpec(memory_space=pltpu.HBM)
    V = pltpu.VMEM
    sem = lambda *shape: pltpu.SemaphoreType.DMA(shape)
    operands = (
        tokens,
        norm_mix.reshape(1, -1),
        routes.T,
        route_w.T,
        norm_ffn.reshape(1, -1),
        gate_vector.reshape(-1, 128),
        state,
        w_query,
        w_key,
        w_value,
        w_out,
        dense_gate.T,
        dense_up.T,
        dense_down,
        exp_gate[0].T,
        exp_up[0].T,
        exp_down,
    )
    held = [pltpu.with_memory_space_constraint(x, pltpu.HBM) for x in operands]
    mixed, new_state = pl.pallas_call(
        functools.partial(kernel, A, B),
        out_shape=(pltpu.VMEM((R, H), BF16), pltpu.VMEM(state.shape, F32)),
        in_specs=[hbm] * 17,
        out_specs=(vm, vm),
        scratch_shapes=[
            V((R, H), BF16),
            V((1, 2 * H), F32),
            V((routes.shape[1], R), jnp.int32),
            V((routes.shape[1], R), BF16),
            V((1, H), F32),
            V((H // 128, 128), BF16),
            V((R, H), BF16),
            V((H // 128, 128), BF16),
            V((2, H, HW), BF16),
            V((2, H, HW), BF16),
            V((2, H, HW), BF16),
            V((2, HW, H), BF16),
            V((2, HW, H), BF16),
            V((2, FD, H), BF16),
            V((2, FD, H), BF16),
            V((FD, H), BF16),
            V((2, FE, H), BF16),
            V((2, FE, H), BF16),
            V((2, FE, H), BF16),
            V(state.shape, F32),
            V((R, HW), BF16),
            V((R, HW), BF16),
            V((B, A, R, 128), BF16),
            V((B, A, R, H), BF16),
            V((B, A, R, H), BF16),
            V((A, R, H), F32),
            V((B, A, R, H), BF16),
            V((B, A, R, H), BF16),
            V((B, A, R, H), BF16),
            V((B, A, R, H), BF16),
            V((A, R, H), BF16),
            V((A, R, H), BF16),
            sem(25),
            sem(7),
            sem(7),
            sem(A),
            sem(A),
            sem(B),
            sem(B),
            sem(A),
            sem(A),
            sem(B, A),
            sem(B, A),
            sem(B, A),
            sem(B, A),
            sem(B),
            sem(B),
            sem(B),
            sem(B),
            sem(A),
            sem(A),
        ],
        compiler_params=pltpu.CompilerParams(
            collective_id=0, has_side_effects=True, vmem_limit_bytes=50 * 1024 * 1024
        ),
        name="layer",
    )(
        *held
    )
    return pl.pallas_call(
        store,
        out_shape=(
            jax.ShapeDtypeStruct((R, H), BF16),
            jax.ShapeDtypeStruct(state.shape, F32),
        ),
        in_specs=[vm, vm],
        out_specs=(hbm, hbm),
        scratch_shapes=[sem(2)],
        name="store",
    )(
        pltpu.with_memory_space_constraint(mixed, pltpu.VMEM),
        pltpu.with_memory_space_constraint(new_state, pltpu.VMEM),
    )


def solution(mesh):
    return jax.shard_map(
        body,
        mesh=mesh,
        in_specs=(
            P("ep", "tp"),
            P("ep", "tp", None, None),
            P(),
            P(None, "tp"),
            P(None, "tp"),
            P(None, "tp"),
            P("tp", None),
            P("tp"),
            P("tp"),
            P("tp", "ep"),
            P("tp", "ep"),
            P("ep", "tp"),
            P("ep", None, "tp"),
            P("ep", None, "tp"),
            P("ep", "tp", None),
            P("ep", None),
            P("ep", None),
        ),
        out_specs=(P("ep", "tp"), P("ep", "tp", None, None)),
        check_vma=False,
    )
```

```python
import functools

import jax
import jax.numpy as jnp
from jax import lax
from jax.experimental import pallas as pl
from jax.experimental.pallas import tpu as pltpu
from jax.sharding import PartitionSpec as P

EXPERTS = 8
ROWS = 256
epsilon = 1e-06
MESH = pl.DeviceIdType.MESH
F32 = jnp.float32
BF16 = jnp.bfloat16


def dot(a, b):
    return jnp.dot(a, b, preferred_element_type=F32)


def dot_t(a, b):
    return lax.dot_general(a, b, (((1,), (1,)), ((), ())), preferred_element_type=F32)


def silu(v):
    return v / (1.0 + jnp.exp(-v))


def kernel(
    A,
    B,
    tokens_h,
    norm_mix_h,
    routes_h,
    route_w_h,
    norm_ffn_h,
    gate_vec_h,
    state,
    w_query,
    w_key,
    w_value,
    w_out,
    dense_gate,
    dense_up,
    dense_down,
    exp_gate,
    exp_up,
    exp_down,
    mixed,
    ns,
    tokens,
    norm_mix,
    routes,
    route_w,
    norm_ffn,
    gate_vec,
    tok_p,
    gvec_p,
    wq,
    wk,
    wv,
    wo_o,
    wo_p,
    dg,
    du,
    dd,
    eg,
    eu,
    ed,
    st,
    ho_o,
    ho_p,
    aux,
    xo,
    xp,
    y0,
    yx_s,
    yx_r,
    ys,
    rsx,
    zs,
    rsz,
    lsem,
    psem_s,
    psem_r,
    axz_s,
    axz_r,
    axx_s,
    axx_r,
    gz_s,
    gz_r,
    gx_s,
    gx_r,
    gp_s,
    gp_r,
    yx_ss,
    yx_rs,
    rx_s,
    rx_r,
    rz_s,
    rz_r,
):
    R, H = tokens.shape
    D = 2 * H
    heads, hs = state.shape[1], state.shape[2]
    HW = heads * hs
    n = A * B
    me = lax.axis_index("ep")
    tp = lax.axis_index("tp")
    z, xy = me // B, me % B
    other = 1 - tp
    expert = me // (n // EXPERTS)
    partner = {"ep": me, "tp": other}
    xpeer = [{"ep": z * B + (xy + j) % B, "tp": tp} for j in range(B)]
    zpeer = [{"ep": ((z + i) % A) * B + xy, "tp": tp} for i in range(A)]

    own_at = pl.multiple_of(tp * H, H)
    oth_at = pl.multiple_of(other * H, H)
    own, oth = pl.ds(own_at, H), pl.ds(oth_at, H)

    sent = []

    def remote(src, dst, s, r, dev):
        copy = pltpu.make_async_remote_copy(
            src_ref=src, dst_ref=dst, send_sem=s, recv_sem=r, device_id=dev, device_id_type=MESH
        )
        copy.start()
        sent.append(copy)
        return copy

    local = {}

    def load(name, k, src, dst):
        copy = pltpu.make_async_copy(src, dst, lsem.at[k])
        copy.start()
        local[name] = copy

    small = (
        (tokens_h, tokens),
        (norm_mix_h, norm_mix),
        (routes_h, routes),
        (route_w_h, route_w),
        (norm_ffn_h, norm_ffn),
        (gate_vec_h, gate_vec),
    )
    barrier = pltpu.get_barrier_semaphore()
    for dev in [partner] + xpeer[1:] + zpeer[1:]:
        pl.semaphore_signal(barrier, inc=1, device_id=dev, device_id_type=MESH)

    for t, (src, dst) in enumerate(small):
        load(f"s{t}", 19 + t, src, dst)
    for t, (src, dst) in enumerate(((w_query, wq), (w_key, wk), (w_value, wv))):
        load(f"p{t}o", 2 * t, src.at[own, :], dst.at[0])
        load(f"p{t}p", 2 * t + 1, src.at[oth, :], dst.at[1])
    load("st", 6, state, st)
    load("wo0", 7, w_out.at[:, own], wo_o.at[0])
    load("wo1", 8, w_out.at[:, oth], wo_o.at[1])
    for t in (2, 3):
        local[f"s{t}"].wait()
    row_id = lax.broadcasted_iota(jnp.int32, (EXPERTS, R), 0)
    wt = jnp.zeros((EXPERTS, R), F32)
    named = routes[...]
    gains = route_w[...].astype(F32)
    for t in range(routes.shape[0]):
        wt = wt + jnp.where(row_id == named[t : t + 1, :], gains[t : t + 1, :], 0.0)
    wt = jnp.concatenate([wt, jnp.zeros((EXPERTS, 128 - R), F32)], axis=1)
    wt = jnp.concatenate([wt, jnp.zeros((128 - EXPERTS, 128), F32)], axis=0)
    aux[0, 0] = wt.T[:R].astype(BF16)

    for t in (0, 1, 4, 5):
        local[f"s{t}"].wait()
    pl.semaphore_wait(barrier, 1 + (B - 1) + (A - 1))

    c_tok = remote(tokens, tok_p, psem_s.at[0], psem_r.at[0], partner)
    c_ext = remote(gate_vec, gvec_p, psem_s.at[1], psem_r.at[1], partner)
    c_wo0 = remote(w_out.at[:, oth], wo_p.at[0], psem_s.at[2], psem_r.at[2], partner)
    c_wo1 = remote(w_out.at[:, own], wo_p.at[1], psem_s.at[3], psem_r.at[3], partner)
    c_dg = remote(dense_gate, dg.at[1], psem_s.at[4], psem_r.at[4], partner)
    c_du = remote(dense_up, du.at[1], psem_s.at[5], psem_r.at[5], partner)
    load("dg", 9, dense_gate, dg.at[0])
    load("du", 10, dense_up, du.at[0])
    load("dd", 11, dense_down, dd)
    load("eg0", 12, exp_gate.at[:, own], eg.at[0])
    load("eu0", 13, exp_up.at[:, own], eu.at[0])
    load("eg1", 14, exp_gate.at[:, oth], eg.at[1])
    load("eu1", 15, exp_up.at[:, oth], eu.at[1])
    load("ed1", 16, exp_down.at[0, :, oth], ed.at[1])
    load("ed0", 17, exp_down.at[0, :, own], ed.at[0])
    c_axz = [None] + [
        remote(aux.at[0, 0], aux.at[A - i, 0], axz_s.at[i], axz_r.at[A - i], zpeer[i])
        for i in range(1, A)
    ]

    tok_f = tokens[...].astype(F32)
    c_tok.wait_recv()
    tok_pf = tok_p[...].astype(F32)
    total = jnp.sum(tok_f * tok_f, axis=1, keepdims=True) + jnp.sum(
        tok_pf * tok_pf, axis=1, keepdims=True
    )
    scale = lax.rsqrt(total / D + epsilon)
    gain_o = norm_mix[:, own]
    gain_p = norm_mix[:, oth]
    nx_o = (tok_f * scale * gain_o).astype(BF16)
    nx_p = (tok_pf * scale * gain_p).astype(BF16)
    proj = []
    for t, w in enumerate((wq, wk, wv)):
        local[f"p{t}o"].wait()
        part = dot(nx_o, w[0])
        local[f"p{t}p"].wait()
        proj.append((part + dot(nx_p, w[1])).astype(BF16).astype(F32))
    q, k, v = proj
    k = k * hs ** (-0.5)
    pad = jnp.zeros((128 - R, HW), F32)
    q_t = jnp.concatenate([q, pad], axis=0).T
    k_t = jnp.concatenate([k, pad], axis=0).T
    head_id = tp * heads
    local["st"].wait()
    decays = []
    for h in range(heads):
        cols = slice(h * hs, (h + 1) * hs)
        idv = jnp.zeros((1, 128), F32) + (head_id + h).astype(F32)
        decay = 1.0 - jnp.exp2(-3.0 - 2.0 * idv)
        decays.append(decay)
        rows = []
        for s in range(R):
            rows.append(jnp.sum(st[s, h] * q_t[cols, s : s + 1], axis=0, keepdims=True))
        qs = jnp.concatenate(rows, axis=0)
        qk = jnp.sum(q[:, cols] * k[:, cols], axis=1, keepdims=True)
        read = decay * qs + qk * v[:, cols]
        centre = jnp.mean(read, axis=1, keepdims=True)
        dev = read - centre
        spread = jnp.mean(dev * dev, axis=1, keepdims=True)
        ho_o[:, cols] = (dev * lax.rsqrt(spread + epsilon)).astype(BF16)
    c_ho = remote(ho_o, ho_p, psem_s.at[6], psem_r.at[6], partner)
    ho = ho_o[...]
    local["wo0"].wait()
    local["wo1"].wait()
    a_o = dot(ho, wo_o[0]).astype(BF16).astype(F32)
    a_p = dot(ho, wo_o[1]).astype(BF16).astype(F32)
    c_wo0.wait_recv()
    c_wo1.wait_recv()
    c_ho.wait_recv()
    hp = ho_p[...]
    a_o = a_o + dot(hp, wo_p[0]).astype(BF16).astype(F32)
    a_p = a_p + dot(hp, wo_p[1]).astype(BF16).astype(F32)
    after = (tok_f + a_o).astype(BF16).astype(F32)
    after_p = (tok_pf + a_p).astype(BF16).astype(F32)
    squares = jnp.sum(after * after, axis=1, keepdims=True) + jnp.sum(
        after_p * after_p, axis=1, keepdims=True
    )
    xo[0, 0] = (after * lax.rsqrt(squares / D + epsilon) * norm_ffn[...]).astype(BF16)

    c_gz = [None] * A
    c_gx = {}
    c_gp = {}
    for i in range(1, A):
        c_gz[i] = remote(xo.at[0, 0], xo.at[A - i, 0], gz_s.at[i], gz_r.at[A - i], zpeer[i])

    def spread_block(i):
        for j in range(1, B):
            c_gx[i, j] = remote(
                xo.at[i, 0], xo.at[i, B - j], gx_s.at[i, j], gx_r.at[i, B - j], xpeer[j]
            )

    def to_partner(i, j):
        c_gp[i, j] = remote(xo.at[i, j], xp.at[i, j], gp_s.at[i, j], gp_r.at[i, j], partner)

    spread_block(0)
    to_partner(0, 0)
    c_axx = {}
    for i in range(A):
        if i > 0:
            c_axz[A - i].wait_recv()
        for j in range(1, B):
            c_axx[i, j] = remote(
                aux.at[i, 0], aux.at[i, B - j], axx_s.at[i, j], axx_r.at[i, B - j], xpeer[j]
            )

    for h in range(heads):
        cols = slice(h * hs, (h + 1) * hs)
        for s in range(R):
            ns[s, h] = decays[h] * st[s, h] + k_t[cols, s : s + 1] * v[s : s + 1, cols]

    order = sorted(range(A), key=lambda i: min(i, A - i))
    for i in order[1:]:
        c_gz[A - i].wait_recv()
        spread_block(i)
        to_partner(i, 0)

    c_ext.wait_recv()
    for name in ("dg", "du", "dd", "eg0", "eu0", "eg1", "eu1", "ed1", "ed0"):
        local[name].wait()
    c_dg.wait_recv()
    c_du.wait_recv()
    group = max(1, min(A, ROWS // (B * R)))
    rows = group * B * R

    def gate_row(ref):
        part = ref[...].astype(F32)
        return jnp.concatenate([part[r : r + 1] for r in range(H // 128)], axis=1)

    gvec_o = gate_row(gate_vec)
    gvec_q = gate_row(gvec_p)
    lanes = lax.broadcasted_iota(jnp.int32, (rows, 128), 1)
    c_yx = {}
    c_rx = {}
    c_rz = {}

    def arrive(i):
        for j in range(1, B):
            c_gx[i, B - j].wait_recv()
            to_partner(i, j)

    def experts(g):
        slots = range(g * group, (g + 1) * group)
        at = slice(g * group, (g + 1) * group)
        for i in slots:
            for j in range(1, B):
                c_axx[i, B - j].wait_recv()
        x_o = xo[at].reshape(rows, H)
        gate = dot_t(x_o, eg[0])
        up = dot_t(x_o, eu[0])
        d_gate = dot_t(x_o, dg[0])
        d_up = dot_t(x_o, du[0])
        logit = jnp.sum(x_o.astype(F32) * gvec_o, axis=1, keepdims=True)
        for i in slots:
            for j in range(B):
                c_gp[i, j].wait_recv()
        x_p = xp[at].reshape(rows, H)
        gate = gate + dot_t(x_p, eg[1])
        up = up + dot_t(x_p, eu[1])
        d_gate = d_gate + dot_t(x_p, dg[1])
        d_up = d_up + dot_t(x_p, du[1])
        logit = logit + jnp.sum(x_p.astype(F32) * gvec_q, axis=1, keepdims=True)
        table = aux[at].reshape(rows, 128).astype(F32)
        weight = jnp.sum(jnp.where(lanes == expert, table, 0.0), axis=1, keepdims=True)
        hidden = (silu(gate) * up).astype(BF16)
        d_hidden = (1.0 / (1.0 + jnp.exp(-logit)) * silu(d_gate) * d_up).astype(BF16)
        yx_s[at] = (weight * dot(hidden, ed[1])).astype(BF16).reshape(group, B, R, H)
        span = pl.ds(g * group, group)
        c_yx[g] = remote(yx_s.at[span], yx_r.at[span], yx_ss.at[g], yx_rs.at[g], partner)
        y = weight * dot(hidden, ed[0]) + dot(d_hidden, dd[...])
        y0[at] = y.reshape(group, B, R, H)

    def plane_send(g):
        c_yx[g].wait_recv()
        for i in range(g * group, (g + 1) * group):
            y = y0[i] + yx_r[i].astype(F32)
            y0[i, 0] = y[0]
            ys[i] = y.astype(BF16)
            for j in range(1, B):
                c_rx[i, j] = remote(
                    ys.at[i, j], rsx.at[i, B - j], rx_s.at[i, j], rx_r.at[i, B - j], xpeer[j]
                )

    def plane_sum(g):
        for i in range(g * group, (g + 1) * group):
            total = y0[i, 0]
            for j in range(1, B):
                c_rx[i, B - j].wait_recv()
                total = total + rsx[i, j].astype(F32)
            if i == 0:
                y0[0, 0] = total
            else:
                zs[i] = total.astype(BF16)
                c_rz[i] = remote(zs.at[i], rsz.at[A - i], rz_s.at[i], rz_r.at[A - i], zpeer[i])

    turns = A // group
    for t in range(turns + 2):
        if t < turns:
            for i in order:
                if i // group == t:
                    arrive(i)
            experts(t)
        if 1 <= t <= turns:
            plane_send(t - 1)
        if t >= 2:
            plane_sum(t - 2)

    result = after + y0[0, 0]
    for i in range(1, A):
        c_rz[A - i].wait_recv()
        result = result + rsz[i].astype(F32)
    mixed[...] = result.astype(BF16)
    for copy in sent:
        copy.wait_send()


def store(a_in, b_in, a_out, b_out, sems):
    first = pltpu.make_async_copy(b_in, b_out, sems.at[0])
    second = pltpu.make_async_copy(a_in, a_out, sems.at[1])
    first.start()
    second.start()
    first.wait()
    second.wait()


def body(
    tokens,
    state,
    norm_mix,
    w_query,
    w_key,
    w_value,
    w_out,
    norm_ffn,
    gate_vector,
    dense_gate,
    dense_up,
    dense_down,
    exp_gate,
    exp_up,
    exp_down,
    routes,
    route_w,
):
    n = lax.axis_size("ep")
    A = 1
    while (2 * A) * (2 * A) <= n:
        A = 2 * A
    B = n // A
    R, H = tokens.shape
    heads, hs = state.shape[1], state.shape[2]
    HW = heads * hs
    FE = exp_gate.shape[2]
    FD = dense_gate.shape[1]
    vm = pl.BlockSpec(memory_space=pltpu.VMEM)
    hbm = pl.BlockSpec(memory_space=pltpu.HBM)
    V = pltpu.VMEM
    sem = lambda *shape: pltpu.SemaphoreType.DMA(shape)
    operands = (
        tokens,
        norm_mix.reshape(1, -1),
        routes.T,
        route_w.T,
        norm_ffn.reshape(1, -1),
        gate_vector.reshape(-1, 128),
        state,
        w_query,
        w_key,
        w_value,
        w_out,
        dense_gate.T,
        dense_up.T,
        dense_down,
        exp_gate[0].T,
        exp_up[0].T,
        exp_down,
    )
    held = [pltpu.with_memory_space_constraint(x, pltpu.HBM) for x in operands]
    mixed, new_state = pl.pallas_call(
        functools.partial(kernel, A, B),
        out_shape=(pltpu.VMEM((R, H), BF16), pltpu.VMEM(state.shape, F32)),
        in_specs=[hbm] * 17,
        out_specs=(vm, vm),
        scratch_shapes=[
            V((R, H), BF16),
            V((1, 2 * H), F32),
            V((routes.shape[1], R), jnp.int32),
            V((routes.shape[1], R), BF16),
            V((1, H), F32),
            V((H // 128, 128), BF16),
            V((R, H), BF16),
            V((H // 128, 128), BF16),
            V((2, H, HW), BF16),
            V((2, H, HW), BF16),
            V((2, H, HW), BF16),
            V((2, HW, H), BF16),
            V((2, HW, H), BF16),
            V((2, FD, H), BF16),
            V((2, FD, H), BF16),
            V((FD, H), BF16),
            V((2, FE, H), BF16),
            V((2, FE, H), BF16),
            V((2, FE, H), BF16),
            V(state.shape, F32),
            V((R, HW), BF16),
            V((R, HW), BF16),
            V((A, B, R, 128), BF16),
            V((A, B, R, H), BF16),
            V((A, B, R, H), BF16),
            V((A, B, R, H), F32),
            V((A, B, R, H), BF16),
            V((A, B, R, H), BF16),
            V((A, B, R, H), BF16),
            V((A, B, R, H), BF16),
            V((A, R, H), BF16),
            V((A, R, H), BF16),
            sem(25),
            sem(7),
            sem(7),
            sem(A),
            sem(A),
            sem(A, B),
            sem(A, B),
            sem(A),
            sem(A),
            sem(A, B),
            sem(A, B),
            sem(A, B),
            sem(A, B),
            sem(A),
            sem(A),
            sem(A, B),
            sem(A, B),
            sem(A),
            sem(A),
        ],
        compiler_params=pltpu.CompilerParams(
            collective_id=0, has_side_effects=True, vmem_limit_bytes=50 * 1024 * 1024
        ),
        name="layer",
    )(
        *held
    )
    return pl.pallas_call(
        store,
        out_shape=(
            jax.ShapeDtypeStruct((R, H), BF16),
            jax.ShapeDtypeStruct(state.shape, F32),
        ),
        in_specs=[vm, vm],
        out_specs=(hbm, hbm),
        scratch_shapes=[sem(2)],
        name="store",
    )(
        pltpu.with_memory_space_constraint(mixed, pltpu.VMEM),
        pltpu.with_memory_space_constraint(new_state, pltpu.VMEM),
    )


def solution(mesh):
    return jax.shard_map(
        body,
        mesh=mesh,
        in_specs=(
            P("ep", "tp"),
            P("ep", "tp", None, None),
            P(),
            P(None, "tp"),
            P(None, "tp"),
            P(None, "tp"),
            P("tp", None),
            P("tp"),
            P("tp"),
            P("tp", "ep"),
            P("tp", "ep"),
            P("ep", "tp"),
            P("ep", None, "tp"),
            P("ep", None, "tp"),
            P("ep", "tp", None),
            P("ep", None),
            P("ep", None),
        ),
        out_specs=(P("ep", "tp"), P("ep", "tp", None, None)),
        check_vma=False,
    )
```
